32 devices in a mesh: grp: 2 (over x), sp: 4 (over y, core), tp: 4 (over z).
Axes of the slice: x: 2, y: 2, z: 4, core: 2. Of those that a mesh axis runs over, the one named last changes fastest.
Arguments:
- tokens: bfloat16 [8, 1024, 2048], P(('grp', 'tp'), 'sp'), parts along dimension 0, may hold values from -6 to 6
- kv_down: bfloat16 [2048, 512], replicated, may hold values from -0.125 to 0.125
- rope_down: bfloat16 [2048, 64], replicated, may hold values from -0.125 to 0.125
- kv_gain: float32 [512], replicated, may hold values from 0.1 to 1.9
- key_up: bfloat16 [512, 16, 128], replicated, may hold values from -0.25 to 0.25
- value_up: bfloat16 [512, 16, 128], replicated, may hold values from -0.25 to 0.25
- query_nope: bfloat16 [8, 16, 128], P(('grp', 'sp'), 'tp'), parts along dimension 0, may hold values from -180 to 180
- query_rope: bfloat16 [8, 16, 64], P(('grp', 'sp'), 'tp'), parts along dimension 0, may hold values from -180 to 180
Outputs:
- key_cache: bfloat16 [8, 16, 1024, 128], P(('grp', 'sp'), 'tp'), parts along dimension 0
- value_cache: bfloat16 [8, 16, 1024, 128], P(('grp', 'sp'), 'tp'), parts along dimension 0
- rope_cache: bfloat16 [8, 1024, 64], P(('grp', 'sp')), parts along dimension 0
- read_out: bfloat16 [8, 16, 128], P(('grp', 'sp'), 'tp'), parts along dimension 0
The draws below stay inside these ranges and needn't reach their ends.
There are 2 independent parts, one for each index of `grp`. The reference program is written for one: setup_inputs(seed, part) draws one part's arguments, and reference() takes and returns one part's arrays. A program takes and returns all parts, laid end to end along the dimension named above; an argument that names none is the same for every part. Nothing has to cross between parts.
All inputs are finite; a program needn't handle non-finite values.
Results may differ from the reference program's by a relative error of at most 0.018.
The reference program's roundings to bfloat16 on the way (of `normed` and `rotated`) count: a program that leaves them out, or rounds other values in their place, can miss the bound.
Values may be sent and summed in bfloat16 or wider, within the bound.
A program may use at most 64 MiB of HBM per device.

```python
import jax
import jax.numpy as jnp
from jax import lax

D = 2048
HEADS = 16
KVL = 512
NOPE = 128
ROPE = 64
VD = 128
SEQS = 4
LEN = 1024


def query_draw(key, width):
    base = jax.random.normal(jax.random.fold_in(key, 11), (SEQS, HEADS, width), jnp.float32)
    base = jnp.clip(base, -6.0, 6.0)
    return base.astype(jnp.bfloat16)


def draw_query_nope(key, part):
    return query_draw(jax.random.fold_in(key, 1), NOPE)


def draw_query_rope(key, part):
    return query_draw(jax.random.fold_in(key, 2), ROPE)


def steps_of(key, shape, shards, least, high):
    loudness = 1.0
    for dim, blocks in shards:
        heights = jax.random.uniform(jax.random.fold_in(jax.random.fold_in(key, 6), dim), (blocks,), jnp.float32, least / len(shards), high / len(shards))
        loudness = loudness * jnp.repeat(jnp.exp(heights), shape[dim] // blocks).reshape((-1,) + (1,) * (len(shape) - 1 - dim))
    return loudness


def noise(stream_key, shape, scale, limit, pieces=(), kind=jnp.bfloat16):
    values = scale * jax.random.normal(stream_key, shape, jnp.float32)
    if pieces:
        values = values * steps_of(stream_key, shape, pieces, -0.22, 0.18)
    return jnp.clip(values, -limit, limit).astype(kind)


def setup_inputs(seed: int = 0, part: int = 0) -> dict:
    arg_keys = jax.random.split(jax.random.key(seed), 9)
    part_keys = jax.random.split(jax.random.fold_in(arg_keys[8], part), 9)
    return {
        "tokens": noise(part_keys[0], (SEQS, LEN, D), 1.0, 6.0, ((0, 4), (1, 4))),
        "kv_down": noise(arg_keys[1], (D, KVL), D ** -0.5, 0.125),
        "rope_down": noise(arg_keys[2], (D, ROPE), D ** -0.5, 0.125),
        "kv_gain": jnp.clip(1.0 + 0.18 * jax.random.normal(arg_keys[3], (KVL,), jnp.float32), 0.1, 1.9),
        "key_up": noise(arg_keys[4], (KVL, HEADS, NOPE), KVL ** -0.5, 0.25),
        "value_up": noise(arg_keys[5], (KVL, HEADS, VD), KVL ** -0.5, 0.25),
        "query_nope": draw_query_nope(jax.random.fold_in(jax.random.fold_in(arg_keys[8], part), 71), part),
        "query_rope": draw_query_rope(jax.random.fold_in(jax.random.fold_in(arg_keys[8], part), 71), part),
    }


norm_epsilon = 1e-06
rope_base = 10000.0

def rotate(values, positions):
    half_width = values.shape[-1] // 2
    frequency = 1.0 / rope_base ** (jnp.arange(0, 2 * half_width, 2, dtype=jnp.float32) / (2 * half_width))
    angles = positions[..., None] * frequency
    cosine = jnp.cos(angles)
    sine_part = jnp.sin(angles)
    front_half = values[..., :half_width]
    back_half = values[..., half_width:]
    return jnp.concatenate([front_half * cosine - back_half * sine_part, front_half * sine_part + back_half * cosine], axis=-1)

def reference(tokens, kv_down, rope_down, kv_gain, key_up, value_up, query_nope, query_rope):
    positions = jnp.arange(LEN, dtype=jnp.float32)
    key_flat = key_up.reshape(KVL, HEADS * NOPE)
    value_flat = value_up.reshape(KVL, HEADS * VD)

    def one_sequence(seq_rows):
        latent = jnp.dot(seq_rows, kv_down, preferred_element_type=jnp.float32)
        normed = (latent * lax.rsqrt(lax.optimization_barrier(jnp.mean(latent * latent, axis=-1, keepdims=True)) + norm_epsilon) * kv_gain).astype(jnp.bfloat16)
        rope_raw = jnp.dot(seq_rows, rope_down, preferred_element_type=jnp.float32)
        rope_key = rotate(rope_raw, positions).astype(jnp.bfloat16)
        key_rows = jnp.dot(normed, key_flat, preferred_element_type=jnp.float32).astype(jnp.bfloat16)
        value_rows = jnp.dot(normed, value_flat, preferred_element_type=jnp.float32).astype(jnp.bfloat16)
        key_rows = key_rows.reshape(LEN, HEADS, NOPE).transpose(1, 0, 2)
        value_rows = value_rows.reshape(LEN, HEADS, VD).transpose(1, 0, 2)
        return (key_rows, value_rows, rope_key)
    key_cache, value_cache, rope_cache = lax.map(one_sequence, tokens)
    query_pos = jnp.full((HEADS,), LEN, dtype=jnp.float32)
    rotated = rotate(query_rope.astype(jnp.float32), query_pos).astype(jnp.bfloat16)
    score_scale = (NOPE + ROPE) ** (-0.5)
    scores = jnp.einsum('shd,shld->shl', query_nope.astype(jnp.float32), key_cache.astype(jnp.float32))
    scores = scores + jnp.einsum('shr,slr->shl', rotated.astype(jnp.float32), rope_cache.astype(jnp.float32))
    scores = scores * score_scale
    row_max = lax.optimization_barrier(jnp.max(scores, axis=-1, keepdims=True))
    expo_terms = jnp.exp(scores - row_max)
    weights = expo_terms / lax.optimization_barrier(jnp.sum(expo_terms, axis=-1, keepdims=True))
    read_out = jnp.einsum('shl,shld->shd', weights, value_cache.astype(jnp.float32)).astype(jnp.bfloat16)
    return (key_cache, value_cache, rope_cache, read_out)
```

```python
import functools

import jax
import jax.numpy as jnp
import numpy as np
from jax import lax
from jax.experimental import pallas as pl
from jax.experimental.pallas import tpu as pltpu
from jax.sharding import PartitionSpec as P

norm_epsilon = 1e-06
rope_base = 10000.0
MESH = pl.DeviceIdType.MESH
F32, BF16 = jnp.float32, jnp.bfloat16


def tables(length, width):
    frequency = (1.0 / rope_base ** (np.arange(0, width, 2, dtype=np.float64) / width)).astype(np.float32)
    angles = frequency[:, None] * np.arange(length, dtype=np.float32)[None, :]
    cached = np.stack([np.cos(angles.astype(np.float64)), np.sin(angles.astype(np.float64))])
    ask = (np.float32(length) * frequency).astype(np.float64)
    asked = np.stack([np.tile(np.cos(ask), 2), np.tile(np.sin(ask), 2)])
    return cached.astype(np.float32), asked.astype(np.float32)


def kernel(
    sp_count, tp_count, heads_dev, cuts, parts,
    tok, kvd, rpt, gain, kup, vup, tab,
    key_out, val_out, rope_out,
    box, tok_v, kvd_v, rpt_v, gain_v, up_v, wide, kw, vw, tab_v,
    first_sem, in_sem, zsend, zrecv, csend, crecv,
):
    me = lax.axis_index("sp")
    here = lax.axis_index("tp")
    seq_local, pos_dev, model_width = tok.shape
    rope_width = rpt.shape[0]
    half = rope_width // 2
    key_width = kup.shape[2]
    rope_rows = box.shape[1] - pos_dev
    rope_packs = rope_width // rope_rows
    pieces = [pl.ds(a, b - a) for a, b in zip(cuts[:-1], cuts[1:])]
    count = len(pieces)
    last = tp_count - 1
    inner = {0: here < last, 1: here > 0}
    ends = {0: here == last, 1: here == 0}
    near_end = {0: here + 1 == last, 1: here - 1 == 0}
    at_end = jnp.logical_or(here == 0, here == last)

    half_rows = pos_dev // 2
    starts = (0, half_rows + rope_rows)
    halves = ([s for s in range(count) if cuts[s] < half_rows], [s for s in range(count) if cuts[s] >= half_rows])

    barrier = pltpu.get_barrier_semaphore()
    for step in range(1, sp_count):
        pl.semaphore_signal(
            barrier, inc=1, device_id={"sp": lax.rem(me + step, sp_count)}, device_id_type=MESH
        )
    for way in (0, 1):
        @pl.when(inner[way])
        def _(way=way):
            for step in range(sp_count):
                pl.semaphore_signal(
                    barrier, inc=1,
                    device_id={"sp": lax.rem(me + step, sp_count), "tp": here + (1 if way == 0 else -1)},
                    device_id_type=MESH,
                )

    tile = up_v.shape[2]
    head_start = here * heads_dev
    head_tile = pl.multiple_of(head_start // tile * tile, tile)
    head_off = lax.rem(head_start, tile)
    deep = model_width // parts
    firsts = []
    for n in range(parts):
        span = pl.ds(n * deep, deep)
        firsts.append([
            pltpu.make_async_copy(src, dst, first_sem.at[n, m])
            for m, (src, dst) in enumerate([
                (kvd.at[span, :], kvd_v.at[span, :]),
                (tok.at[:, 0:half_rows, span], tok_v.at[:, 0:half_rows, span]),
            ])
        ])
    for pair in firsts:
        for load in pair:
            load.start()
    loads = [
        pltpu.make_async_copy(src, dst, in_sem.at[n])
        for n, (src, dst) in enumerate([
            (gain, gain_v),
            (tok.at[:, half_rows:pos_dev, :], tok_v.at[:, half_rows:pos_dev, :]),
            (rpt, rpt_v),
            (tab.at[:, :, pl.ds(pl.multiple_of(me * pos_dev, pos_dev), pos_dev)], tab_v),
            (kup.at[:, pl.ds(head_tile, tile), :], up_v.at[0]),
            (vup.at[:, pl.ds(head_tile, tile), :], up_v.at[1]),
        ])
    ]
    for load in loads:
        load.start()

    def slot(prompt):
        return jnp.where(prompt == me, me, sp_count + prompt)

    def along(prompt, way, hop, q, s, final=False):
        part = box.at[slot(prompt), pieces[s]]
        tp = here + (1 if way == 0 else -1)
        if final:
            return pltpu.make_async_remote_copy(
                src_ref=part, dst_ref=box.at[me, pieces[s]],
                send_sem=zsend.at[way, hop, q, s], recv_sem=crecv.at[me, s],
                device_id={"sp": prompt, "tp": tp}, device_id_type=MESH,
            )
        return pltpu.make_async_remote_copy(
            src_ref=part, dst_ref=part,
            send_sem=zsend.at[way, hop, q, s], recv_sem=zrecv.at[way, hop, q, s],
            device_id={"sp": me, "tp": tp}, device_id_type=MESH,
        )

    def pass_on(prompt, way, hop, q, s):
        final = near_end[way] if hop else jnp.logical_and(near_end[way], prompt == me)

        @pl.when(jnp.logical_and(inner[way], final))
        def _():
            along(prompt, way, hop, q, s, True).start()

        @pl.when(jnp.logical_and(inner[way], jnp.logical_not(final)))
        def _():
            along(prompt, way, hop, q, s).start()

    def across(prompt, s):
        return pltpu.make_async_remote_copy(
            src_ref=box.at[slot(prompt), pieces[s]], dst_ref=box.at[me, pieces[s]],
            send_sem=csend.at[prompt, s], recv_sem=crecv.at[me, s],
            device_id={"sp": prompt}, device_id_type=MESH,
        )

    def normed(latent):
        return (
            latent
            * lax.rsqrt(jnp.mean(latent * latent, axis=-1, keepdims=True) + norm_epsilon)
            * gain_v[...]
        ).astype(BF16)

    def send(group):
        for s in halves[group]:
            for q in range(seq_local):
                prompt = here * seq_local + q
                for way in (0, 1):
                    pass_on(prompt, way, 0, q, s)

                @pl.when(prompt != me)
                def _(s=s):
                    across(prompt, s).start()

    sums = [None] * seq_local
    for n in range(parts):
        for load in firsts[n]:
            load.wait()
        for q in range(seq_local):
            term = jnp.dot(
                tok_v[q, 0:half_rows, n * deep:(n + 1) * deep], kvd_v[n * deep:(n + 1) * deep, :],
                preferred_element_type=F32,
            )
            sums[q] = term if n == 0 else sums[q] + term
    loads[0].wait()
    for q in range(seq_local):
        box[slot(here * seq_local + q), 0:half_rows, :] = normed(sums[q])
    neighbours = jnp.where(here < last, 1, 0) + jnp.where(here > 0, 1, 0)
    pl.semaphore_wait(barrier, sp_count - 1 + sp_count * neighbours)
    send(0)

    for n in (1, 2, 3):
        loads[n].wait()
    for q in range(seq_local):
        mine = slot(here * seq_local + q)
        latent = jnp.dot(tok_v[q, half_rows:pos_dev, :], kvd_v[...], preferred_element_type=F32)
        box[mine, starts[1]:starts[1] + half_rows, :] = normed(latent)
        raw = lax.dot_general(rpt_v[...], tok_v[q], (((1,), (1,)), ((), ())), preferred_element_type=F32)
        cosine, sine_part = tab_v[0], tab_v[1]
        front, back = raw[:half], raw[half:]
        turned = jnp.concatenate(
            [front * cosine - back * sine_part, front * sine_part + back * cosine], axis=0
        ).astype(BF16)
        box[mine, half_rows:half_rows + rope_rows, :] = jnp.concatenate(
            [turned[g * rope_rows:(g + 1) * rope_rows] for g in range(rope_packs)], axis=1
        )
    send(1)

    for n in (4, 5):
        loads[n].wait()
    depth = up_v.shape[1]
    for n, target in enumerate((kw, vw)):
        wide[...] = up_v[n].astype(F32).reshape(depth * tile, key_width)
        for h in range(heads_dev):
            target[:, h * key_width:(h + 1) * key_width] = wide[
                pl.ds(head_off + h, depth, stride=tile), :
            ].astype(BF16)

    for hop in range(last):
        for s in range(count):
            for q in range(seq_local):
                for way in (1, 0):
                    owner = here - 1 - hop if way == 0 else here + 1 + hop
                    prompt = owner * seq_local + q
                    has = owner >= 0 if way == 0 else owner <= last
                    landed = ends[way] if hop else jnp.logical_and(ends[way], prompt == me)

                    @pl.when(jnp.logical_and(has, jnp.logical_not(landed)))
                    def _(way=way, prompt=prompt):
                        along(prompt, way, hop, q, s).wait_recv()
                        if hop + 1 < last:
                            pass_on(prompt, way, hop + 1, q, s)

                        @pl.when(prompt != me)
                        def _():
                            across(prompt, s).start()

    def arrived(source, s):
        part = box.at[source, pieces[s]]
        pltpu.make_async_remote_copy(
            src_ref=part, dst_ref=part,
            send_sem=csend.at[source, s], recv_sem=crecv.at[source, s],
            device_id={"sp": source}, device_id_type=MESH,
        ).wait_recv()

    home = me // seq_local == here
    for group in range(2):
        for step in range(sp_count):
            source = lax.rem(me + step, sp_count)
            for s in halves[group]:
                if step:
                    arrived(source, s)
                else:
                    @pl.when(jnp.logical_and(at_end, jnp.logical_not(home)))
                    def _(s=s):
                        arrived(me, s)
            if group == 1:
                block = pl.ds(pl.multiple_of(source * pos_dev, pos_dev), pos_dev)
                packed = box[source, half_rows:half_rows + rope_rows, :]
                rope_out[0, :, block] = jnp.concatenate(
                    [packed[:, g * pos_dev:(g + 1) * pos_dev] for g in range(rope_packs)], axis=0
                )
            rows = box[source, starts[group]:starts[group] + half_rows, :]
            place = pl.ds(pl.multiple_of(source * pos_dev + group * half_rows, half_rows), half_rows)
            keys = jnp.dot(rows, kw[...], preferred_element_type=F32).astype(BF16)
            values = jnp.dot(rows, vw[...], preferred_element_type=F32).astype(BF16)
            for h in range(heads_dev):
                key_out[0, h, place, :] = keys[:, h * key_width:(h + 1) * key_width]
                val_out[0, h, place, :] = values[:, h * key_width:(h + 1) * key_width]

    for hop in range(last):
        for q in range(seq_local):
            for s in range(count):
                for way in (0, 1):
                    owner = here - hop if way == 0 else here + hop
                    has = owner >= 0 if way == 0 else owner <= last

                    @pl.when(jnp.logical_and(has, inner[way]))
                    def _(way=way, s=s, owner=owner):
                        along(owner * seq_local + q, way, hop, q, s).wait_send()
    for step in range(1, sp_count):
        prompt = lax.rem(me + step, sp_count)
        far = jnp.abs(prompt // seq_local - here) > 1

        @pl.when(jnp.logical_not(jnp.logical_and(at_end, far)))
        def _(prompt=prompt):
            for s in range(count):
                across(prompt, s).wait_send()


def finish(scale, keys, vals, ropes, query, ask, qtab, key_out, val_out, rope_out, read_out, sem):
    heads_dev, key_width = query.shape[1], query.shape[2]
    moves = [pltpu.make_async_copy(ropes, rope_out, sem.at[2, 0])]
    for n, (src, dst) in enumerate([(keys, key_out), (vals, val_out)]):
        for h in range(heads_dev):
            moves.append(pltpu.make_async_copy(src.at[:, h], dst.at[:, h], sem.at[n, h]))
    for move in moves:
        move.start()
    half = ask.shape[2] // 2
    turn = ask[0].astype(F32)
    swapped = jnp.concatenate([-turn[:, half:], turn[:, :half]], axis=1)
    rotated = (turn * qtab[0:1, :] + swapped * qtab[1:2, :]).astype(BF16)
    shape = (heads_dev, heads_dev * key_width)
    own = lax.broadcasted_iota(jnp.int32, shape, 1) // key_width == lax.broadcasted_iota(jnp.int32, shape, 0)
    spread = jnp.where(own, jnp.concatenate([query[0].astype(F32)] * heads_dev, axis=1), 0.0).astype(BF16)
    all_keys = jnp.concatenate([keys[0, h] for h in range(heads_dev)], axis=1)
    total = lax.dot_general(spread, all_keys, (((1,), (1,)), ((), ())), preferred_element_type=F32)
    total = (total + jnp.dot(rotated, ropes[0], preferred_element_type=F32)) * scale
    terms = jnp.exp(total - jnp.max(total, axis=-1, keepdims=True))
    weights = terms / jnp.sum(terms, axis=-1, keepdims=True)
    high = weights.astype(BF16).astype(F32)
    both = jnp.concatenate([high, weights - high], axis=0).astype(BF16)
    all_vals = jnp.concatenate([vals[0, h] for h in range(heads_dev)], axis=1)
    reads = jnp.dot(both, all_vals, preferred_element_type=F32)
    picks = []
    for h in range(heads_dev):
        span = slice(h * key_width, (h + 1) * key_width)
        picks.append(reads[h:h + 1, span] + reads[heads_dev + h:heads_dev + h + 1, span])
    read_out[0] = jnp.concatenate(picks, axis=0).astype(BF16)
    for move in moves:
        move.wait()


def local(tokens, kv_down, rope_down, kv_gain, key_up, value_up, query_nope, query_rope):
    seq_local, pos_dev, model_width = tokens.shape
    sp_count = lax.axis_size("sp")
    tp_count = lax.axis_size("tp")
    latent_width = kv_down.shape[1]
    rope_width = rope_down.shape[1]
    head_count, key_width = key_up.shape[1], key_up.shape[2]
    heads_dev = head_count // tp_count
    length = pos_dev * sp_count
    rope_rows = rope_width * pos_dev // latent_width
    rows = rope_rows + pos_dev
    quarter = pos_dev // 4
    cuts = (0, quarter, 2 * quarter, 3 * quarter + rope_rows, rows)
    parts = 4
    prompts = tp_count * seq_local
    cached, asked = tables(length, rope_width)
    tile = 8
    any_space = pl.BlockSpec(memory_space=pl.ANY)
    hbm = pl.BlockSpec(memory_space=pltpu.HBM)
    vmem = pl.BlockSpec(memory_space=pltpu.VMEM)
    hops = max(tp_count - 1, 1)
    count = len(cuts) - 1
    dma = pltpu.SemaphoreType.DMA
    made = pl.pallas_call(
        functools.partial(kernel, sp_count, tp_count, heads_dev, cuts, parts),
        out_shape=(
            jax.ShapeDtypeStruct((1, heads_dev, length, key_width), BF16),
            jax.ShapeDtypeStruct((1, heads_dev, length, key_width), BF16),
            jax.ShapeDtypeStruct((1, rope_width, length), BF16),
        ),
        in_specs=[hbm] * 7,
        out_specs=(vmem,) * 3,
        scratch_shapes=[
            pltpu.VMEM((sp_count + prompts, rows, latent_width), BF16),
            pltpu.VMEM(tokens.shape, BF16),
            pltpu.VMEM(kv_down.shape, BF16),
            pltpu.VMEM((rope_width, model_width), BF16),
            pltpu.VMEM((1, latent_width), F32),
            pltpu.VMEM((2, latent_width, tile, key_width), BF16),
            pltpu.VMEM((latent_width * tile, key_width), F32),
            pltpu.VMEM((latent_width, heads_dev * key_width), BF16),
            pltpu.VMEM((latent_width, heads_dev * key_width), BF16),
            pltpu.VMEM((2, rope_width // 2, pos_dev), F32),
            dma((parts, 2)),
            dma((6,)),
            dma((2, hops, seq_local, count)),
            dma((2, hops, seq_local, count)),
            dma((prompts, count)),
            dma((sp_count, count)),
        ],
        compiler_params=pltpu.CompilerParams(
            collective_id=0, has_side_effects=True, vmem_limit_bytes=53000000
        ),
    )(
        *[
            pltpu.with_memory_space_constraint(array, pltpu.HBM)
            for array in (
                tokens, kv_down, rope_down.T, kv_gain.reshape(1, latent_width), key_up, value_up,
                jnp.asarray(cached),
            )
        ]
    )
    key_cache, value_cache, rope_t, read_out = pl.pallas_call(
        functools.partial(finish, (key_width + rope_width) ** (-0.5)),
        out_shape=tuple(jax.ShapeDtypeStruct(part.shape, BF16) for part in made)
        + (jax.ShapeDtypeStruct((1, heads_dev, key_width), BF16),),
        in_specs=[vmem] * 6,
        out_specs=(any_space,) * 3 + (vmem,),
        scratch_shapes=[dma((3, heads_dev))],
        compiler_params=pltpu.CompilerParams(vmem_limit_bytes=8 * 1024 * 1024),
    )(*made, query_nope, query_rope, jnp.asarray(asked))
    return (key_cache, value_cache, jnp.swapaxes(rope_t, 1, 2), read_out)


def solution(mesh):
    placed = (
        P(("grp", "tp"), "sp", None),
        P(),
        P(),
        P(),
        P(),
        P(),
        P(("grp", "sp"), "tp", None),
        P(("grp", "sp"), "tp", None),
    )
    return jax.shard_map(
        local,
        mesh=mesh,
        in_specs=placed,
        out_specs=(
            P(("grp", "sp"), "tp", None, None),
            P(("grp", "sp"), "tp", None, None),
            P(("grp", "sp"), None, None),
            P(("grp", "sp"), "tp", None),
        ),
        check_vma=False,
    )
```

```python
import functools

import jax
import jax.numpy as jnp
import numpy as np
from jax import lax
from jax.experimental import pallas as pl
from jax.experimental.pallas import tpu as pltpu
from jax.sharding import PartitionSpec as P

norm_epsilon = 1e-06
rope_base = 10000.0
MESH = pl.DeviceIdType.MESH
F32, BF16 = jnp.float32, jnp.bfloat16


def tables(length, width):
    frequency = (1.0 / rope_base ** (np.arange(0, width, 2, dtype=np.float64) / width)).astype(np.float32)
    angles = frequency[:, None] * np.arange(length, dtype=np.float32)[None, :]
    cached = np.stack([np.cos(angles.astype(np.float64)), np.sin(angles.astype(np.float64))])
    ask = (np.float32(length) * frequency).astype(np.float64)
    asked = np.stack([np.tile(np.cos(ask), 2), np.tile(np.sin(ask), 2)])
    return cached.astype(np.float32), asked.astype(np.float32)


def kernel(
    sp_count, tp_count, heads_dev, cuts, groups, parts,
    tok, kvd, rpt, gain, kup, vup, tab,
    key_out, val_out, rope_out,
    box, tok_v, kvd_v, rpt_v, gain_v, up_v, wide, kw, vw, tab_v,
    first_sem, in_sem, sent, zrecv, crecv,
):
    me = lax.axis_index("sp")
    here = lax.axis_index("tp")
    seq_local, pos_dev, model_width = tok.shape
    rope_width = rpt.shape[0]
    half = rope_width // 2
    key_width = kup.shape[2]
    rope_rows = box.shape[1] - pos_dev
    rope_packs = rope_width // rope_rows
    pieces = [pl.ds(a, b - a) for a, b in zip(cuts[:-1], cuts[1:])]
    count = len(pieces)
    last = tp_count - 1
    inner = {0: here < last, 1: here > 0}
    ends = {0: here == last, 1: here == 0}
    near_end = {0: here + 1 == last, 1: here - 1 == 0}
    at_end = jnp.logical_or(here == 0, here == last)

    half_rows = pos_dev // 2
    halves = ([s for s in range(count) if cuts[s] < half_rows], [s for s in range(count) if cuts[s] >= half_rows])
    spans = [pl.ds(cuts[g[0]], cuts[g[-1] + 1] - cuts[g[0]]) for g in groups]
    group_of = {s: n for n, g in enumerate(groups) for s in g}

    tile = up_v.shape[2]
    head_start = here * heads_dev
    head_tile = pl.multiple_of(head_start // tile * tile, tile)
    head_off = lax.rem(head_start, tile)
    deep = model_width // parts
    firsts = []
    for n in range(parts):
        span = pl.ds(n * deep, deep)
        firsts.append([
            pltpu.make_async_copy(src, dst, first_sem.at[n, m])
            for m, (src, dst) in enumerate([
                (kvd.at[span, :], kvd_v.at[span, :]),
                (tok.at[:, 0:half_rows, span], tok_v.at[:, 0:half_rows, span]),
            ])
        ])
    for pair in firsts:
        for load in pair:
            load.start()
    loads = [
        pltpu.make_async_copy(src, dst, in_sem.at[n])
        for n, (src, dst) in enumerate([
            (gain, gain_v),
            (tok.at[:, half_rows:pos_dev, :], tok_v.at[:, half_rows:pos_dev, :]),
            (rpt, rpt_v),
            (tab.at[:, :, pl.ds(pl.multiple_of(me * pos_dev, pos_dev), pos_dev)], tab_v),
        ])
    ]
    ups = [
        pltpu.make_async_copy(src.at[:, pl.ds(head_tile, tile), :], up_v.at[n], in_sem.at[4])
        for n, src in enumerate((kup, vup))
    ]
    for load in loads + ups:
        load.start()

    barrier = pltpu.get_barrier_semaphore()
    for way in (0, 1):
        @pl.when(inner[way])
        def _(way=way):
            pl.semaphore_signal(
                barrier, inc=1, device_id={"tp": here + (1 if way == 0 else -1)}, device_id_type=MESH
            )
    for step in range(1, sp_count):
        pl.semaphore_signal(
            barrier, inc=1, device_id={"sp": lax.rem(me + step, sp_count)}, device_id_type=MESH
        )
    for way in (0, 1):
        @pl.when(jnp.logical_and(ends[way], inner[1 - way]))
        def _(way=way):
            for step in range(1, sp_count):
                pl.semaphore_signal(
                    barrier, inc=1,
                    device_id={"sp": lax.rem(me + step, sp_count), "tp": here + (-1 if way == 0 else 1)},
                    device_id_type=MESH,
                )

    def greeted():
        total = sp_count - 1
        for way in (0, 1):
            total = total + jnp.where(inner[way], jnp.where(near_end[way], sp_count, 1), 0)
        pl.semaphore_wait(barrier, total)

    def slot(prompt):
        return jnp.where(prompt == me, me, sp_count + prompt)

    def along(prompt, way, s, final=False):
        part = box.at[slot(prompt), pieces[s]]
        tp = here + (1 if way == 0 else -1)
        if final:
            return pltpu.make_async_remote_copy(
                src_ref=part, dst_ref=box.at[me, pieces[s]],
                send_sem=sent.at[0], recv_sem=crecv.at[me, group_of[s]],
                device_id={"sp": prompt, "tp": tp}, device_id_type=MESH,
            )
        return pltpu.make_async_remote_copy(
            src_ref=part, dst_ref=part,
            send_sem=sent.at[0], recv_sem=zrecv.at[prompt, s],
            device_id={"sp": me, "tp": tp}, device_id_type=MESH,
        )

    def pass_on(prompt, way, hop, s):
        final = near_end[way] if hop else jnp.logical_and(near_end[way], prompt == me)

        @pl.when(jnp.logical_and(inner[way], final))
        def _():
            along(prompt, way, s, True).start()

        @pl.when(jnp.logical_and(inner[way], jnp.logical_not(final)))
        def _():
            along(prompt, way, s).start()

    def across(prompt, s):
        return pltpu.make_async_remote_copy(
            src_ref=box.at[slot(prompt), pieces[s]], dst_ref=box.at[me, pieces[s]],
            send_sem=sent.at[1], recv_sem=crecv.at[me, group_of[s]],
            device_id={"sp": prompt}, device_id_type=MESH,
        )

    def normed(latent):
        return (
            latent
            * lax.rsqrt(jnp.mean(latent * latent, axis=-1, keepdims=True) + norm_epsilon)
            * gain_v[...]
        ).astype(BF16)

    def send(group):
        for s in halves[group]:
            for q in range(seq_local):
                prompt = here * seq_local + q
                for way in (0, 1):
                    pass_on(prompt, way, 0, s)

                @pl.when(prompt != me)
                def _(s=s):
                    across(prompt, s).start()

    sums = [None] * seq_local
    for n in range(parts):
        for load in firsts[n]:
            load.wait()
        for q in range(seq_local):
            term = jnp.dot(
                tok_v[q, 0:half_rows, n * deep:(n + 1) * deep], kvd_v[n * deep:(n + 1) * deep, :],
                preferred_element_type=F32,
            )
            sums[q] = term if n == 0 else sums[q] + term
    loads[0].wait()
    for q in range(seq_local):
        box[slot(here * seq_local + q), 0:half_rows, :] = normed(sums[q])
    greeted()
    send(0)

    for n in (1, 2, 3):
        loads[n].wait()
    for q in range(seq_local):
        mine = slot(here * seq_local + q)
        latent = jnp.dot(tok_v[q, half_rows:pos_dev, :], kvd_v[...], preferred_element_type=F32)
        box[mine, half_rows + rope_rows:pos_dev + rope_rows, :] = normed(latent)
        raw = lax.dot_general(rpt_v[...], tok_v[q], (((1,), (1,)), ((), ())), preferred_element_type=F32)
        cosine, sine_part = tab_v[0], tab_v[1]
        front, back = raw[:half], raw[half:]
        turned = jnp.concatenate(
            [front * cosine - back * sine_part, front * sine_part + back * cosine], axis=0
        ).astype(BF16)
        box[mine, half_rows:half_rows + rope_rows, :] = jnp.concatenate(
            [turned[g * rope_rows:(g + 1) * rope_rows] for g in range(rope_packs)], axis=1
        )
    send(1)

    pltpu.make_async_copy(up_v, up_v, in_sem.at[4]).wait()
    depth = up_v.shape[1]
    for n, target in enumerate((kw, vw)):
        wide[...] = up_v[n].astype(F32).reshape(depth * tile, key_width)
        for h in range(heads_dev):
            target[:, h * key_width:(h + 1) * key_width] = wide[
                pl.ds(head_off + h, depth, stride=tile), :
            ].astype(BF16)

    for hop in range(last):
        for s in range(count):
            for q in range(seq_local):
                for way in (1, 0):
                    owner = here - 1 - hop if way == 0 else here + 1 + hop
                    prompt = owner * seq_local + q
                    has = owner >= 0 if way == 0 else owner <= last
                    landed = ends[way] if hop else jnp.logical_and(ends[way], prompt == me)

                    @pl.when(jnp.logical_and(has, jnp.logical_not(landed)))
                    def _(way=way, prompt=prompt):
                        along(prompt, way, s).wait_recv()
                        if hop + 1 < last:
                            pass_on(prompt, way, hop + 1, s)

                        @pl.when(prompt != me)
                        def _():
                            across(prompt, s).start()

    def arrived(source, group):
        part = box.at[source, spans[group]]
        pltpu.make_async_remote_copy(
            src_ref=part, dst_ref=part, send_sem=sent.at[1], recv_sem=crecv.at[source, group],
            device_id={"sp": source}, device_id_type=MESH,
        ).wait_recv()

    home = me // seq_local == here
    for group, members in enumerate(groups):
        begin, stop = cuts[members[0]], cuts[members[-1] + 1]
        with_rope = begin <= half_rows < stop
        if with_rope:
            begin = begin + rope_rows
        height = stop - begin
        first = begin if begin < half_rows else begin - rope_rows
        batch = max(pos_dev // height, 1)
        for base in range(0, sp_count, batch):
            steps = range(base, min(base + batch, sp_count))
            sources = [lax.rem(me + step, sp_count) for step in steps]
            for step, source in zip(steps, sources):
                if step:
                    arrived(source, group)
                else:
                    @pl.when(jnp.logical_and(at_end, jnp.logical_not(home)))
                    def _():
                        arrived(me, group)
                if with_rope:
                    block = pl.ds(pl.multiple_of(source * pos_dev, pos_dev), pos_dev)
                    packed = box[source, half_rows:half_rows + rope_rows, :]
                    rope_out[0, :, block] = jnp.concatenate(
                        [packed[:, g * pos_dev:(g + 1) * pos_dev] for g in range(rope_packs)], axis=0
                    )
            rows = jnp.concatenate([box[source, begin:stop, :] for source in sources], axis=0)
            for weight, target in ((kw, key_out), (vw, val_out)):
                made = jnp.dot(rows, weight[...], preferred_element_type=F32).astype(BF16)
                for n, source in enumerate(sources):
                    place = pl.ds(pl.multiple_of(source * pos_dev + first, height), height)
                    for h in range(heads_dev):
                        target[0, h, place, :] = made[
                            n * height:(n + 1) * height, h * key_width:(h + 1) * key_width
                        ]

    def drain(index, blocks, most):
        for n in range(1, most + 1):
            @pl.when(blocks == n)
            def _(n=n):
                part = box.at[0:n]
                pltpu.make_async_remote_copy(
                    src_ref=part, dst_ref=part, send_sem=sent.at[index], recv_sem=crecv.at[0, 0],
                    device_id={"sp": me}, device_id_type=MESH,
                ).wait_send()

    upward = jnp.where(inner[0], (here + 1) * seq_local, 0)
    downward = jnp.where(inner[1], (tp_count - here) * seq_local, 0)
    drain(0, upward + downward, (tp_count + 1) * seq_local if tp_count > 1 else 0)
    prompts = tp_count * seq_local
    beside = jnp.logical_or(jnp.logical_not(at_end), jnp.abs(me // seq_local - here) <= 1)
    reach = jnp.where(at_end, min(tp_count, 2) * seq_local, prompts)
    drain(1, reach - jnp.where(beside, 1, 0), prompts)


def finish(scale, keys, vals, ropes, query, ask, qtab, key_out, val_out, rope_out, read_out, read, sem):
    heads_dev, key_width = query.shape[1], query.shape[2]
    moves = [
        pltpu.make_async_copy(src, dst, sem.at[n])
        for n, (src, dst) in enumerate([(keys, key_out), (vals, val_out), (ropes, rope_out)])
    ]
    for move in moves:
        move.start()
    half = ask.shape[2] // 2
    turn = ask[0].astype(F32)
    swapped = jnp.concatenate([-turn[:, half:], turn[:, :half]], axis=1)
    rotated = (turn * qtab[0:1, :] + swapped * qtab[1:2, :]).astype(BF16)
    shape = (heads_dev, heads_dev * key_width)
    own = lax.broadcasted_iota(jnp.int32, shape, 1) // key_width == lax.broadcasted_iota(jnp.int32, shape, 0)
    spread = jnp.where(own, jnp.concatenate([query[0].astype(F32)] * heads_dev, axis=1), 0.0).astype(BF16)
    all_keys = jnp.concatenate([keys[0, h] for h in range(heads_dev)], axis=1)
    total = lax.dot_general(spread, all_keys, (((1,), (1,)), ((), ())), preferred_element_type=F32)
    total = (total + jnp.dot(rotated, ropes[0], preferred_element_type=F32)) * scale
    terms = jnp.exp(total - jnp.max(total, axis=-1, keepdims=True))
    weights = terms / jnp.sum(terms, axis=-1, keepdims=True)
    high = weights.astype(BF16).astype(F32)
    both = jnp.concatenate([high, weights - high], axis=0).astype(BF16)
    all_vals = jnp.concatenate([vals[0, h] for h in range(heads_dev)], axis=1)
    reads = jnp.dot(both, all_vals, preferred_element_type=F32)
    picks = []
    for h in range(heads_dev):
        span = slice(h * key_width, (h + 1) * key_width)
        picks.append(reads[h:h + 1, span] + reads[heads_dev + h:heads_dev + h + 1, span])
    read[0] = jnp.concatenate(picks, axis=0).astype(BF16)
    moves.append(pltpu.make_async_copy(read, read_out, sem.at[3]))
    moves[-1].start()
    for move in moves:
        move.wait()


def local(tokens, kv_down, rope_down, kv_gain, key_up, value_up, query_nope, query_rope):
    seq_local, pos_dev, model_width = tokens.shape
    sp_count = lax.axis_size("sp")
    tp_count = lax.axis_size("tp")
    latent_width = kv_down.shape[1]
    rope_width = rope_down.shape[1]
    head_count, key_width = key_up.shape[1], key_up.shape[2]
    heads_dev = head_count // tp_count
    length = pos_dev * sp_count
    rope_rows = rope_width * pos_dev // latent_width
    rows = rope_rows + pos_dev
    quarter = pos_dev // 4
    cuts = (0, quarter, 2 * quarter, 3 * quarter + rope_rows, rows)
    groups = ((0, 1), (2,), (3,))
    parts = 4
    prompts = tp_count * seq_local
    cached, asked = tables(length, rope_width)
    tile = 8
    any_space = pl.BlockSpec(memory_space=pl.ANY)
    hbm = pl.BlockSpec(memory_space=pltpu.HBM)
    vmem = pl.BlockSpec(memory_space=pltpu.VMEM)
    count = len(cuts) - 1
    dma = pltpu.SemaphoreType.DMA
    made = pl.pallas_call(
        functools.partial(kernel, sp_count, tp_count, heads_dev, cuts, groups, parts),
        out_shape=(
            jax.ShapeDtypeStruct((1, heads_dev, length, key_width), BF16),
            jax.ShapeDtypeStruct((1, heads_dev, length, key_width), BF16),
            jax.ShapeDtypeStruct((1, rope_width, length), BF16),
        ),
        in_specs=[hbm] * 7,
        out_specs=(vmem,) * 3,
        scratch_shapes=[
            pltpu.VMEM((sp_count + prompts, rows, latent_width), BF16),
            pltpu.VMEM(tokens.shape, BF16),
            pltpu.VMEM(kv_down.shape, BF16),
            pltpu.VMEM((rope_width, model_width), BF16),
            pltpu.VMEM((1, latent_width), F32),
            pltpu.VMEM((2, latent_width, tile, key_width), BF16),
            pltpu.VMEM((latent_width * tile, key_width), F32),
            pltpu.VMEM((latent_width, heads_dev * key_width), BF16),
            pltpu.VMEM((latent_width, heads_dev * key_width), BF16),
            pltpu.VMEM((2, rope_width // 2, pos_dev), F32),
            dma((parts, 2)),
            dma((5,)),
            dma((2,)),
            dma((prompts, count)),
            dma((sp_count, len(groups))),
        ],
        compiler_params=pltpu.CompilerParams(
            collective_id=0, has_side_effects=True, vmem_limit_bytes=53000000
        ),
    )(
        *[
            pltpu.with_memory_space_constraint(array, pltpu.HBM)
            for array in (
                tokens, kv_down, rope_down.T, kv_gain.reshape(1, latent_width), key_up, value_up,
                jnp.asarray(cached),
            )
        ]
    )
    key_cache, value_cache, rope_t, read_out = pl.pallas_call(
        functools.partial(finish, (key_width + rope_width) ** (-0.5)),
        out_shape=tuple(jax.ShapeDtypeStruct(part.shape, BF16) for part in made)
        + (jax.ShapeDtypeStruct((1, heads_dev, key_width), BF16),),
        in_specs=[vmem] * 6,
        out_specs=(any_space,) * 4,
        scratch_shapes=[pltpu.VMEM((1, heads_dev, key_width), BF16), dma((4,))],
        compiler_params=pltpu.CompilerParams(vmem_limit_bytes=8 * 1024 * 1024),
    )(*made, query_nope, query_rope, jnp.asarray(asked))
    return (key_cache, value_cache, jnp.swapaxes(rope_t, 1, 2), read_out)


def solution(mesh):
    placed = (
        P(("grp", "tp"), "sp", None),
        P(),
        P(),
        P(),
        P(),
        P(),
        P(("grp", "sp"), "tp", None),
        P(("grp", "sp"), "tp", None),
    )
    return jax.shard_map(
        local,
        mesh=mesh,
        in_specs=placed,
        out_specs=(
            P(("grp", "sp"), "tp", None, None),
            P(("grp", "sp"), "tp", None, None),
            P(("grp", "sp"), None, None),
            P(("grp", "sp"), "tp", None),
        ),
        check_vma=False,
    )
```

```python
import functools

import jax
import jax.numpy as jnp
import numpy as np
from jax import lax
from jax.experimental import pallas as pl
from jax.experimental.pallas import tpu as pltpu
from jax.sharding import PartitionSpec as P

norm_epsilon = 1e-06
rope_base = 10000.0
MESH = pl.DeviceIdType.MESH
F32, BF16 = jnp.float32, jnp.bfloat16


def tables(length, width):
    frequency = (1.0 / rope_base ** (np.arange(0, width, 2, dtype=np.float64) / width)).astype(np.float32)
    angles = frequency[:, None] * np.arange(length, dtype=np.float32)[None, :]
    cached = np.stack([np.cos(angles.astype(np.float64)), np.sin(angles.astype(np.float64))])
    ask = (np.float32(length) * frequency).astype(np.float64)
    asked = np.stack([np.tile(np.cos(ask), 2), np.tile(np.sin(ask), 2)])
    return cached.astype(np.float32), asked.astype(np.float32)


def kernel(
    sp_count, tp_count, heads_dev, lead, rope_at, cuts, groups, parts,
    tok, kvd, rpt, gain, kup, vup, tab,
    key_out, val_out, rope_out,
    box, tok_v, kvd_v, rpt_v, gain_v, up_v, wide, kw, vw, tab_v,
    load_sem, sent, zrecv, crecv, ready,
):
    me = lax.axis_index("sp")
    here = lax.axis_index("tp")
    seq_local, pos_dev, model_width = tok.shape
    latent_width = kvd.shape[1]
    rope_width = rpt.shape[0]
    half = rope_width // 2
    key_width = kup.shape[2]
    rope_rows = box.shape[1] - pos_dev
    rope_packs = rope_width // rope_rows
    pieces = [pl.ds(a, b - a) for a, b in zip(cuts[:-1], cuts[1:])]
    count = len(pieces)
    last = tp_count - 1
    prompts = tp_count * seq_local
    inner = {0: here < last, 1: here > 0}
    ends = {0: here == last, 1: here == 0}
    near_end = {0: here + 1 == last, 1: here - 1 == 0}
    at_end = jnp.logical_or(here == 0, here == last)

    spans = [pl.ds(cuts[g[0]], cuts[g[-1] + 1] - cuts[g[0]]) for g in groups]
    group_of = {s: n for n, g in enumerate(groups) for s in g}

    tile = up_v.shape[2]
    head_start = here * heads_dev
    head_tile = pl.multiple_of(head_start // tile * tile, tile)
    head_off = lax.rem(head_start, tile)
    deep = model_width // parts

    def load(pairs, index):
        size = 0
        for src, dst in pairs:
            pltpu.make_async_copy(src, dst, load_sem.at[index]).start()
            size += int(np.prod(dst.shape)) * dst.dtype.itemsize
        rows = size // (latent_width * kvd_v.dtype.itemsize)
        whole = kvd_v.at[0:rows, :]
        return pltpu.make_async_copy(whole, whole, load_sem.at[index])

    firsts = []
    for n in range(parts):
        span = pl.ds(n * deep, deep)
        firsts.append(load([
            (kvd.at[span, :], kvd_v.at[span, :]),
            (tok.at[:, 0:lead, span], tok_v.at[:, 0:lead, span]),
        ], n))
    gains = pltpu.make_async_copy(gain, gain_v, load_sem.at[parts])
    gains.start()
    rest = load([
        (tok.at[:, lead:pos_dev, :], tok_v.at[:, lead:pos_dev, :]),
        (rpt, rpt_v),
        (tab.at[:, :, pl.ds(pl.multiple_of(me * pos_dev, pos_dev), pos_dev)], tab_v),
    ], parts + 1)
    for n, src in enumerate((kup, vup)):
        pltpu.make_async_copy(
            src.at[:, pl.ds(head_tile, tile), :], up_v.at[n], load_sem.at[parts + 2]
        ).start()

    lanes = [*range(1, sp_count, 2), *range(0, sp_count, 2)]
    barrier = pltpu.get_barrier_semaphore()
    for way in (0, 1):
        @pl.when(inner[way])
        def _(way=way):
            pl.semaphore_signal(
                barrier, inc=1, device_id={"tp": here + (1 if way == 0 else -1)}, device_id_type=MESH
            )
    for step in range(1, sp_count):
        pl.semaphore_signal(
            barrier, inc=1, device_id={"sp": lax.rem(me + step, sp_count)}, device_id_type=MESH
        )

    def slot(prompt):
        return jnp.where(prompt == me, me, sp_count + prompt)

    def along(prompt, way, s, final=False):
        part = box.at[slot(prompt), pieces[s]]
        tp = here + (1 if way == 0 else -1)
        if final:
            return pltpu.make_async_remote_copy(
                src_ref=part, dst_ref=box.at[me, pieces[s]],
                send_sem=sent.at[0], recv_sem=crecv.at[me, group_of[s]],
                device_id={"sp": prompt, "tp": tp}, device_id_type=MESH,
            )
        return pltpu.make_async_remote_copy(
            src_ref=part, dst_ref=part,
            send_sem=sent.at[0], recv_sem=zrecv.at[prompt, s],
            device_id={"sp": me, "tp": tp}, device_id_type=MESH,
        )

    def pass_on(prompt, way, hop, s):
        final = near_end[way] if hop else jnp.logical_and(near_end[way], prompt == me)

        @pl.when(jnp.logical_and(inner[way], final))
        def _():
            along(prompt, way, s, True).start()

        @pl.when(jnp.logical_and(inner[way], jnp.logical_not(final)))
        def _():
            along(prompt, way, s).start()

    def across(prompt, s):
        return pltpu.make_async_remote_copy(
            src_ref=box.at[slot(prompt), pieces[s]], dst_ref=box.at[me, pieces[s]],
            send_sem=sent.at[1], recv_sem=crecv.at[me, group_of[s]],
            device_id={"sp": prompt}, device_id_type=MESH,
        )

    def normed(latent):
        return (
            latent
            * lax.rsqrt(jnp.mean(latent * latent, axis=-1, keepdims=True) + norm_epsilon)
            * gain_v[...]
        ).astype(BF16)

    def send(chosen):
        for s in chosen:
            for q in range(seq_local):
                prompt = here * seq_local + q
                for way in (1, 0):
                    pass_on(prompt, way, 0, s)

                @pl.when(prompt != me)
                def _(s=s):
                    across(prompt, s).start()

    sums = [None] * seq_local
    for n in range(parts):
        firsts[n].wait()
        for q in range(seq_local):
            term = jnp.dot(
                tok_v[q, 0:lead, n * deep:(n + 1) * deep], kvd_v[n * deep:(n + 1) * deep, :],
                preferred_element_type=F32,
            )
            sums[q] = term if n == 0 else sums[q] + term
    gains.wait()
    for q in range(seq_local):
        box[slot(here * seq_local + q), 0:lead, :] = normed(sums[q])
    pl.semaphore_wait(
        barrier, sp_count - 1 + jnp.where(inner[0], 1, 0) + jnp.where(inner[1], 1, 0)
    )
    send((0,))

    for way in (0, 1):
        @pl.when(jnp.logical_and(ends[way], inner[1 - way]))
        def _(way=way):
            pl.semaphore_signal(
                ready.at[0], inc=1, device_id={"tp": here + (-1 if way == 0 else 1)}, device_id_type=MESH
            )

    def finish_rows(begin, stop, place):
        for q in range(seq_local):
            latent = jnp.dot(tok_v[q, begin:stop, :], kvd_v[...], preferred_element_type=F32)
            box[slot(here * seq_local + q), place:place + stop - begin, :] = normed(latent)

    rest.wait()
    finish_rows(lead, rope_at, lead)
    send((1,))
    finish_rows(rope_at, pos_dev, rope_at + rope_rows)
    for q in range(seq_local):
        raw = lax.dot_general(rpt_v[...], tok_v[q], (((1,), (1,)), ((), ())), preferred_element_type=F32)
        cosine, sine_part = tab_v[0], tab_v[1]
        front, back = raw[:half], raw[half:]
        turned = jnp.concatenate(
            [front * cosine - back * sine_part, front * sine_part + back * cosine], axis=0
        ).astype(BF16)
        box[slot(here * seq_local + q), rope_at:rope_at + rope_rows, :] = jnp.concatenate(
            [turned[g * rope_rows:(g + 1) * rope_rows] for g in range(rope_packs)], axis=1
        )
    send(range(2, count))

    pltpu.make_async_copy(up_v, up_v, load_sem.at[parts + 2]).wait()
    depth = up_v.shape[1]
    for n, target in enumerate((kw, vw)):
        wide[...] = up_v[n].astype(F32).reshape(depth * tile, key_width)
        for h in range(heads_dev):
            target[:, h * key_width:(h + 1) * key_width] = wide[
                pl.ds(head_off + h, depth, stride=tile), :
            ].astype(BF16)

    for way in (0, 1):
        @pl.when(jnp.logical_and(inner[way], near_end[way]))
        def _():
            pl.semaphore_wait(ready.at[0], 1)

    for hop in range(last):
        for s in range(count):
            for q in range(seq_local):
                for way in (1, 0):
                    owner = here - 1 - hop if way == 0 else here + 1 + hop
                    prompt = owner * seq_local + q
                    has = owner >= 0 if way == 0 else owner <= last
                    landed = ends[way] if hop else jnp.logical_and(ends[way], prompt == me)

                    @pl.when(jnp.logical_and(has, jnp.logical_not(landed)))
                    def _(way=way, prompt=prompt):
                        along(prompt, way, s).wait_recv()
                        if hop + 1 < last:
                            pass_on(prompt, way, hop + 1, s)

                        @pl.when(prompt != me)
                        def _():
                            across(prompt, s).start()

    def arrived(source, group):
        part = box.at[source, spans[group]]
        pltpu.make_async_remote_copy(
            src_ref=part, dst_ref=part, send_sem=sent.at[1], recv_sem=crecv.at[source, group],
            device_id={"sp": me}, device_id_type=MESH,
        ).wait_recv()

    landed = jnp.logical_and(at_end, me // seq_local != here)
    for group, members in enumerate(groups):
        begin, stop = cuts[members[0]], cuts[members[-1] + 1]
        with_rope = begin <= rope_at < stop
        ranges = [(begin, rope_at), (rope_at + rope_rows, stop)] if with_rope else [(begin, stop)]
        ranges = [(a, b) for a, b in ranges if b > a]
        height = sum(b - a for a, b in ranges)
        first = begin if begin <= rope_at else begin - rope_rows
        batch = 4 if group == len(groups) - 1 else 2
        for base in range(0, sp_count, batch):
            sources = lanes[base:base + batch]
            for source in sources:
                @pl.when(jnp.logical_or(me != source, landed))
                def _(source=source):
                    arrived(source, group)
                if with_rope:
                    packed = box[source, rope_at:rope_at + rope_rows, :]
                    rope_out[0, :, source * pos_dev:(source + 1) * pos_dev] = jnp.concatenate(
                        [packed[:, g * pos_dev:(g + 1) * pos_dev] for g in range(rope_packs)], axis=0
                    )
            rows = jnp.concatenate([box[source, a:b, :] for source in sources for a, b in ranges], axis=0)
            for weight, target in ((kw, key_out), (vw, val_out)):
                made = jnp.dot(rows, weight[...], preferred_element_type=F32).astype(BF16)
                for n, source in enumerate(sources):
                    place = slice(source * pos_dev + first, source * pos_dev + first + height)
                    for h in range(heads_dev):
                        target[0, h, place, :] = made[
                            n * height:(n + 1) * height, h * key_width:(h + 1) * key_width
                        ]

    def drain(index, blocks, most):
        for n in range(1, most + 1):
            @pl.when(blocks == n)
            def _(n=n):
                part = box.at[0:n]
                pltpu.make_async_remote_copy(
                    src_ref=part, dst_ref=part, send_sem=sent.at[index], recv_sem=zrecv.at[0, 0],
                    device_id={"sp": me}, device_id_type=MESH,
                ).wait_send()

    upward = jnp.where(inner[0], (here + 1) * seq_local, 0)
    downward = jnp.where(inner[1], (tp_count - here) * seq_local, 0)
    drain(0, upward + downward, (tp_count + 1) * seq_local if tp_count > 1 else 0)
    beside = jnp.logical_or(jnp.logical_not(at_end), jnp.abs(me // seq_local - here) <= 1)
    reach = jnp.where(at_end, min(tp_count, 2) * seq_local, prompts)
    drain(1, reach - jnp.where(beside, 1, 0), prompts)


def finish(scale, keys, vals, ropes, query, ask, qtab, key_out, val_out, rope_out, read_out, read, sem):
    heads_dev, key_width = query.shape[1], query.shape[2]
    moves = [
        pltpu.make_async_copy(src, dst, sem.at[n])
        for n, (src, dst) in enumerate([(keys, key_out), (vals, val_out), (ropes, rope_out)])
    ]
    for move in moves:
        move.start()
    half = ask.shape[2] // 2
    turn = ask[0].astype(F32)
    swapped = jnp.concatenate([-turn[:, half:], turn[:, :half]], axis=1)
    rotated = (turn * qtab[0:1, :] + swapped * qtab[1:2, :]).astype(BF16)
    shape = (heads_dev, heads_dev * key_width)
    own = lax.broadcasted_iota(jnp.int32, shape, 1) // key_width == lax.broadcasted_iota(jnp.int32, shape, 0)
    spread = jnp.where(own, jnp.concatenate([query[0].astype(F32)] * heads_dev, axis=1), 0.0).astype(BF16)
    all_keys = jnp.concatenate([keys[0, h] for h in range(heads_dev)], axis=1)
    total = lax.dot_general(spread, all_keys, (((1,), (1,)), ((), ())), preferred_element_type=F32)
    total = (total + jnp.dot(rotated, ropes[0], preferred_element_type=F32)) * scale
    terms = jnp.exp(total - jnp.max(total, axis=-1, keepdims=True))
    high = terms.astype(BF16).astype(F32)
    both = jnp.concatenate([high, terms - high], axis=0).astype(BF16)
    all_vals = jnp.concatenate([vals[0, h] for h in range(heads_dev)], axis=1)
    reads = jnp.dot(both, all_vals, preferred_element_type=F32)
    picks = []
    for h in range(heads_dev):
        span = slice(h * key_width, (h + 1) * key_width)
        picks.append(reads[h:h + 1, span] + reads[heads_dev + h:heads_dev + h + 1, span])
    read[0] = (jnp.concatenate(picks, axis=0) / jnp.sum(terms, axis=-1, keepdims=True)).astype(BF16)
    moves.append(pltpu.make_async_copy(read, read_out, sem.at[3]))
    moves[-1].start()
    for move in moves:
        move.wait()


def local(tokens, kv_down, rope_down, kv_gain, key_up, value_up, query_nope, query_rope):
    seq_local, pos_dev, model_width = tokens.shape
    sp_count = lax.axis_size("sp")
    tp_count = lax.axis_size("tp")
    latent_width = kv_down.shape[1]
    rope_width = rope_down.shape[1]
    head_count, key_width = key_up.shape[1], key_up.shape[2]
    heads_dev = head_count // tp_count
    length = pos_dev * sp_count
    rope_rows = rope_width * pos_dev // latent_width
    rows = rope_rows + pos_dev
    quarter = pos_dev // 4
    lead, rope_at = quarter, 2 * quarter
    cuts = (0, lead, rope_at, rows - quarter // 2, rows)
    groups = ((0, 1), (2,), (3,))
    parts = 4
    prompts = tp_count * seq_local
    cached, asked = tables(length, rope_width)
    tile = 8
    any_space = pl.BlockSpec(memory_space=pl.ANY)
    hbm = pl.BlockSpec(memory_space=pltpu.HBM)
    vmem = pl.BlockSpec(memory_space=pltpu.VMEM)
    count = len(cuts) - 1
    dma = pltpu.SemaphoreType.DMA
    made = pl.pallas_call(
        functools.partial(kernel, sp_count, tp_count, heads_dev, lead, rope_at, cuts, groups, parts),
        out_shape=(
            jax.ShapeDtypeStruct((1, heads_dev, length, key_width), BF16),
            jax.ShapeDtypeStruct((1, heads_dev, length, key_width), BF16),
            jax.ShapeDtypeStruct((1, rope_width, length), BF16),
        ),
        in_specs=[hbm] * 7,
        out_specs=(vmem,) * 3,
        scratch_shapes=[
            pltpu.VMEM((sp_count + prompts, rows, latent_width), BF16),
            pltpu.VMEM(tokens.shape, BF16),
            pltpu.VMEM(kv_down.shape, BF16),
            pltpu.VMEM((rope_width, model_width), BF16),
            pltpu.VMEM((1, latent_width), F32),
            pltpu.VMEM((2, latent_width, tile, key_width), BF16),
            pltpu.VMEM((latent_width * tile, key_width), F32),
            pltpu.VMEM((latent_width, heads_dev * key_width), BF16),
            pltpu.VMEM((latent_width, heads_dev * key_width), BF16),
            pltpu.VMEM((2, rope_width // 2, pos_dev), F32),
            dma((parts + 3,)),
            dma((2,)),
            dma((prompts, count)),
            dma((sp_count, len(groups))),
            pltpu.SemaphoreType.REGULAR((1,)),
        ],
        compiler_params=pltpu.CompilerParams(
            collective_id=0, has_side_effects=True, vmem_limit_bytes=53000000
        ),
    )(
        *[
            pltpu.with_memory_space_constraint(array, pltpu.HBM)
            for array in (
                tokens, kv_down, rope_down.T, kv_gain.reshape(1, latent_width), key_up, value_up,
                jnp.asarray(cached),
            )
        ]
    )
    key_cache, value_cache, rope_t, read_out = pl.pallas_call(
        functools.partial(finish, (key_width + rope_width) ** (-0.5)),
        out_shape=tuple(jax.ShapeDtypeStruct(part.shape, BF16) for part in made)
        + (jax.ShapeDtypeStruct((1, heads_dev, key_width), BF16),),
        in_specs=[vmem] * 6,
        out_specs=(any_space,) * 4,
        scratch_shapes=[pltpu.VMEM((1, heads_dev, key_width), BF16), dma((4,))],
        compiler_params=pltpu.CompilerParams(vmem_limit_bytes=8 * 1024 * 1024),
    )(*made, query_nope, query_rope, jnp.asarray(asked))
    return (key_cache, value_cache, jnp.swapaxes(rope_t, 1, 2), read_out)


def solution(mesh):
    placed = (
        P(("grp", "tp"), "sp", None),
        P(),
        P(),
        P(),
        P(),
        P(),
        P(("grp", "sp"), "tp", None),
        P(("grp", "sp"), "tp", None),
    )
    return jax.shard_map(
        local,
        mesh=mesh,
        in_specs=placed,
        out_specs=(
            P(("grp", "sp"), "tp", None, None),
            P(("grp", "sp"), "tp", None, None),
            P(("grp", "sp"), None, None),
            P(("grp", "sp"), "tp", None),
        ),
        check_vma=False,
    )
```

```python
import functools

import jax
import jax.numpy as jnp
import numpy as np
from jax import lax
from jax.experimental import pallas as pl
from jax.experimental.pallas import tpu as pltpu
from jax.sharding import PartitionSpec as P

norm_epsilon = 1e-06
rope_base = 10000.0
MESH = pl.DeviceIdType.MESH
F32, BF16 = jnp.float32, jnp.bfloat16


def tables(length, width):
    frequency = (1.0 / rope_base ** (np.arange(0, width, 2, dtype=np.float64) / width)).astype(np.float32)
    angles = frequency[:, None] * np.arange(length, dtype=np.float32)[None, :]
    cached = np.stack([np.cos(angles.astype(np.float64)), np.sin(angles.astype(np.float64))])
    ask = (np.float32(length) * frequency).astype(np.float64)
    asked = np.stack([np.tile(np.cos(ask), 2), np.tile(np.sin(ask), 2)])
    return cached.astype(np.float32), asked.astype(np.float32)


def kernel(
    sp_count, tp_count, heads_dev, lead, rope_at, cuts, groups, parts,
    tok, kvd, rpt, gain, kup, vup, tab,
    key_out, val_out, rope_out,
    box, tok_v, kvd_v, rpt_v, gain_v, up_v, wide, kw, vw, tab_v,
    load_sem, sent, zrecv, crecv, ready,
):
    me = lax.axis_index("sp")
    here = lax.axis_index("tp")
    seq_local, pos_dev, model_width = tok.shape
    latent_width = kvd.shape[1]
    rope_width = rpt.shape[0]
    half = rope_width // 2
    key_width = kup.shape[2]
    rope_rows = box.shape[1] - pos_dev
    rope_packs = rope_width // rope_rows
    pieces = [pl.ds(a, b - a) for a, b in zip(cuts[:-1], cuts[1:])]
    count = len(pieces)
    last = tp_count - 1
    prompts = tp_count * seq_local
    inner = {0: here < last, 1: here > 0}
    ends = {0: here == last, 1: here == 0}
    near_end = {0: here + 1 == last, 1: here - 1 == 0}
    at_end = jnp.logical_or(here == 0, here == last)

    spans = [pl.ds(cuts[g[0]], cuts[g[-1] + 1] - cuts[g[0]]) for g in groups]
    group_of = {s: n for n, g in enumerate(groups) for s in g}

    tile = up_v.shape[2]
    head_start = here * heads_dev
    head_tile = pl.multiple_of(head_start // tile * tile, tile)
    head_off = lax.rem(head_start, tile)
    deep = model_width // parts

    def load(pairs, index):
        size = 0
        for src, dst in pairs:
            pltpu.make_async_copy(src, dst, load_sem.at[index]).start()
            size += int(np.prod(dst.shape)) * dst.dtype.itemsize
        rows = size // (latent_width * kvd_v.dtype.itemsize)
        whole = kvd_v.at[0:rows, :]
        return pltpu.make_async_copy(whole, whole, load_sem.at[index])

    firsts = []
    for n in range(parts):
        span = pl.ds(n * deep, deep)
        firsts.append(load([
            (kvd.at[span, :], kvd_v.at[span, :]),
            (tok.at[:, 0:lead, span], tok_v.at[:, 0:lead, span]),
        ], n))
    gains = pltpu.make_async_copy(gain, gain_v, load_sem.at[parts])
    gains.start()
    rest = load([
        (tok.at[:, lead:pos_dev, :], tok_v.at[:, lead:pos_dev, :]),
        (rpt, rpt_v),
        (tab.at[:, :, pl.ds(pl.multiple_of(me * pos_dev, pos_dev), pos_dev)], tab_v),
    ], parts + 1)
    for n, src in enumerate((kup, vup)):
        pltpu.make_async_copy(
            src.at[:, pl.ds(head_tile, tile), :], up_v.at[n], load_sem.at[parts + 2]
        ).start()

    lanes = [*range(1, sp_count, 2), *range(0, sp_count, 2)]
    barrier = pltpu.get_barrier_semaphore()
    for way in (0, 1):
        @pl.when(inner[way])
        def _(way=way):
            pl.semaphore_signal(
                barrier, inc=1, device_id={"tp": here + (1 if way == 0 else -1)}, device_id_type=MESH
            )
    for step in range(1, sp_count):
        pl.semaphore_signal(
            barrier, inc=1, device_id={"sp": lax.rem(me + step, sp_count)}, device_id_type=MESH
        )

    def landing(lane, group):
        return crecv.at[group + lax.rem(lane, 2) if group == 1 else group + (group > 1)]

    def slot(prompt):
        return jnp.where(prompt == me, me, sp_count + prompt)

    def along(prompt, way, s, final=False):
        part = box.at[slot(prompt), pieces[s]]
        tp = here + (1 if way == 0 else -1)
        if final:
            return pltpu.make_async_remote_copy(
                src_ref=part, dst_ref=box.at[me, pieces[s]],
                send_sem=sent.at[0], recv_sem=landing(me, group_of[s]),
                device_id={"sp": prompt, "tp": tp}, device_id_type=MESH,
            )
        return pltpu.make_async_remote_copy(
            src_ref=part, dst_ref=part,
            send_sem=sent.at[0], recv_sem=zrecv.at[prompt - way * seq_local, s],
            device_id={"sp": me, "tp": tp}, device_id_type=MESH,
        )

    def pass_on(prompt, way, hop, s):
        final = near_end[way] if hop else jnp.logical_and(near_end[way], prompt == me)

        @pl.when(jnp.logical_and(inner[way], final))
        def _():
            along(prompt, way, s, True).start()

        @pl.when(jnp.logical_and(inner[way], jnp.logical_not(final)))
        def _():
            along(prompt, way, s).start()

    def across(prompt, s):
        return pltpu.make_async_remote_copy(
            src_ref=box.at[slot(prompt), pieces[s]], dst_ref=box.at[me, pieces[s]],
            send_sem=sent.at[1], recv_sem=landing(me, group_of[s]),
            device_id={"sp": prompt}, device_id_type=MESH,
        )

    def normed(latent):
        return (
            latent
            * lax.rsqrt(jnp.mean(latent * latent, axis=-1, keepdims=True) + norm_epsilon)
            * gain_v[...]
        ).astype(BF16)

    def send(chosen):
        for s in chosen:
            for q in range(seq_local):
                prompt = here * seq_local + q
                for way in (1, 0):
                    pass_on(prompt, way, 0, s)

                @pl.when(prompt != me)
                def _(s=s):
                    across(prompt, s).start()

    sums = [None] * seq_local
    for n in range(parts):
        firsts[n].wait()
        for q in range(seq_local):
            term = jnp.dot(
                tok_v[q, 0:lead, n * deep:(n + 1) * deep], kvd_v[n * deep:(n + 1) * deep, :],
                preferred_element_type=F32,
            )
            sums[q] = term if n == 0 else sums[q] + term
    gains.wait()
    for q in range(seq_local):
        box[slot(here * seq_local + q), 0:lead, :] = normed(sums[q])
    pl.semaphore_wait(
        barrier, sp_count - 1 + jnp.where(inner[0], 1, 0) + jnp.where(inner[1], 1, 0)
    )
    send((0,))

    for way in (0, 1):
        @pl.when(jnp.logical_and(ends[way], inner[1 - way]))
        def _(way=way):
            pl.semaphore_signal(
                ready.at[0], inc=1, device_id={"tp": here + (-1 if way == 0 else 1)}, device_id_type=MESH
            )

    def finish_rows(begin, stop, place):
        for q in range(seq_local):
            latent = jnp.dot(tok_v[q, begin:stop, :], kvd_v[...], preferred_element_type=F32)
            box[slot(here * seq_local + q), place:place + stop - begin, :] = normed(latent)

    rest.wait()
    finish_rows(lead, rope_at, lead)
    send((1,))
    finish_rows(rope_at, pos_dev, rope_at + rope_rows)
    for q in range(seq_local):
        raw = lax.dot_general(rpt_v[...], tok_v[q], (((1,), (1,)), ((), ())), preferred_element_type=F32)
        cosine, sine_part = tab_v[0], tab_v[1]
        front, back = raw[:half], raw[half:]
        turned = jnp.concatenate(
            [front * cosine - back * sine_part, front * sine_part + back * cosine], axis=0
        ).astype(BF16)
        box[slot(here * seq_local + q), rope_at:rope_at + rope_rows, :] = jnp.concatenate(
            [turned[g * rope_rows:(g + 1) * rope_rows] for g in range(rope_packs)], axis=1
        )
    send(range(2, count))

    pltpu.make_async_copy(up_v, up_v, load_sem.at[parts + 2]).wait()
    depth = up_v.shape[1]
    for n, target in enumerate((kw, vw)):
        wide[...] = up_v[n].astype(F32).reshape(depth * tile, key_width)
        for h in range(heads_dev):
            target[:, h * key_width:(h + 1) * key_width] = wide[
                pl.ds(head_off + h, depth, stride=tile), :
            ].astype(BF16)

    for way in (0, 1):
        @pl.when(jnp.logical_and(inner[way], near_end[way]))
        def _():
            pl.semaphore_wait(ready.at[0], 1)

    for hop in range(last):
        for s in range(count):
            for q in range(seq_local):
                for way in (1, 0):
                    owner = here - 1 - hop if way == 0 else here + 1 + hop
                    prompt = owner * seq_local + q
                    has = owner >= 0 if way == 0 else owner <= last
                    landed = ends[way] if hop else jnp.logical_and(ends[way], prompt == me)

                    @pl.when(jnp.logical_and(has, jnp.logical_not(landed)))
                    def _(way=way, prompt=prompt):
                        along(prompt, way, s).wait_recv()
                        if hop + 1 < last:
                            pass_on(prompt, way, hop + 1, s)

                        @pl.when(prompt != me)
                        def _():
                            across(prompt, s).start()

    def arrived(members, group):
        def wait(blocks):
            part = box.at[0:blocks, spans[group]]
            pltpu.make_async_remote_copy(
                src_ref=part, dst_ref=part, send_sem=sent.at[1], recv_sem=landing(members[0], group),
                device_id={"sp": me}, device_id_type=MESH,
            ).wait_recv()

        size = len(members)
        own = lax.rem(me, 2) == members[0] % 2 if group == 1 else me >= 0
        every = jnp.logical_or(landed, jnp.logical_not(own))

        @pl.when(every)
        def _():
            wait(size)
        if size > 1:
            @pl.when(jnp.logical_not(every))
            def _():
                wait(size - 1)

    landed = jnp.logical_and(at_end, me // seq_local != here)
    for group, members in enumerate(groups):
        begin, stop = cuts[members[0]], cuts[members[-1] + 1]
        with_rope = begin <= rope_at < stop
        ranges = [(begin, rope_at), (rope_at + rope_rows, stop)] if with_rope else [(begin, stop)]
        ranges = [(a, b) for a, b in ranges if b > a]
        height = sum(b - a for a, b in ranges)
        first = begin if begin <= rope_at else begin - rope_rows
        batch = 4 if group == len(groups) - 1 else 2
        odds = [lane for lane in lanes if lane % 2]
        evens = [lane for lane in lanes if lane % 2 == 0]
        for base in range(0, sp_count, batch):
            sources = lanes[base:base + batch]
            if group != 1 and base == 0:
                arrived(lanes, group)
            if group == 1 and odds[0] in sources:
                arrived(odds, group)
            if group == 1 and evens[0] in sources:
                arrived(evens, group)
            for source in sources:
                if with_rope:
                    packed = box[source, rope_at:rope_at + rope_rows, :]
                    rope_out[0, :, source * pos_dev:(source + 1) * pos_dev] = jnp.concatenate(
                        [packed[:, g * pos_dev:(g + 1) * pos_dev] for g in range(rope_packs)], axis=0
                    )
            rows = jnp.concatenate([box[source, a:b, :] for source in sources for a, b in ranges], axis=0)
            for weight, target in ((kw, key_out), (vw, val_out)):
                made = jnp.dot(rows, weight[...], preferred_element_type=F32).astype(BF16)
                for n, source in enumerate(sources):
                    place = slice(source * pos_dev + first, source * pos_dev + first + height)
                    for h in range(heads_dev):
                        target[0, h, place, :] = made[
                            n * height:(n + 1) * height, h * key_width:(h + 1) * key_width
                        ]

    def drain(index, blocks, most):
        for n in range(1, most + 1):
            @pl.when(blocks == n)
            def _(n=n):
                part = box.at[0:n]
                pltpu.make_async_remote_copy(
                    src_ref=part, dst_ref=part, send_sem=sent.at[index], recv_sem=zrecv.at[0, 0],
                    device_id={"sp": me}, device_id_type=MESH,
                ).wait_send()

    upward = jnp.where(inner[0], (here + 1) * seq_local, 0)
    downward = jnp.where(inner[1], (tp_count - here) * seq_local, 0)
    drain(0, upward + downward, (tp_count + 1) * seq_local if tp_count > 1 else 0)
    beside = jnp.logical_or(jnp.logical_not(at_end), jnp.abs(me // seq_local - here) <= 1)
    reach = jnp.where(at_end, min(tp_count, 2) * seq_local, prompts)
    drain(1, reach - jnp.where(beside, 1, 0), prompts)


def finish(scale, keys, vals, ropes, query, ask, qtab, key_out, val_out, rope_out, read_out, read, sem):
    heads_dev, key_width = query.shape[1], query.shape[2]
    moves = [
        pltpu.make_async_copy(src, dst, sem.at[n])
        for n, (src, dst) in enumerate([(keys, key_out), (vals, val_out), (ropes, rope_out)])
    ]
    for move in moves:
        move.start()
    half = ask.shape[2] // 2
    turn = ask[0].astype(F32)
    swapped = jnp.concatenate([-turn[:, half:], turn[:, :half]], axis=1)
    rotated = (turn * qtab[0:1, :] + swapped * qtab[1:2, :]).astype(BF16)
    shape = (heads_dev, heads_dev * key_width)
    own = lax.broadcasted_iota(jnp.int32, shape, 1) // key_width == lax.broadcasted_iota(jnp.int32, shape, 0)
    spread = jnp.where(own, jnp.concatenate([query[0].astype(F32)] * heads_dev, axis=1), 0.0).astype(BF16)
    all_keys = jnp.concatenate([keys[0, h] for h in range(heads_dev)], axis=1)
    total = lax.dot_general(spread, all_keys, (((1,), (1,)), ((), ())), preferred_element_type=F32)
    total = (total + jnp.dot(rotated, ropes[0], preferred_element_type=F32)) * scale
    terms = jnp.exp(total - jnp.max(total, axis=-1, keepdims=True))
    high = terms.astype(BF16).astype(F32)
    both = jnp.concatenate([high, terms - high], axis=0).astype(BF16)
    all_vals = jnp.concatenate([vals[0, h] for h in range(heads_dev)], axis=1)
    reads = jnp.dot(both, all_vals, preferred_element_type=F32)
    picks = []
    for h in range(heads_dev):
        span = slice(h * key_width, (h + 1) * key_width)
        picks.append(reads[h:h + 1, span] + reads[heads_dev + h:heads_dev + h + 1, span])
    read[0] = (jnp.concatenate(picks, axis=0) / jnp.sum(terms, axis=-1, keepdims=True)).astype(BF16)
    moves.append(pltpu.make_async_copy(read, read_out, sem.at[3]))
    moves[-1].start()
    for move in moves:
        move.wait()


def local(tokens, kv_down, rope_down, kv_gain, key_up, value_up, query_nope, query_rope):
    seq_local, pos_dev, model_width = tokens.shape
    sp_count = lax.axis_size("sp")
    tp_count = lax.axis_size("tp")
    latent_width = kv_down.shape[1]
    rope_width = rope_down.shape[1]
    head_count, key_width = key_up.shape[1], key_up.shape[2]
    heads_dev = head_count // tp_count
    length = pos_dev * sp_count
    rope_rows = rope_width * pos_dev // latent_width
    rows = rope_rows + pos_dev
    quarter = pos_dev // 4
    lead, rope_at = quarter, 2 * quarter
    cuts = (0, lead, rope_at, rows - quarter // 2, rows)
    groups = ((0, 1), (2,), (3,))
    parts = 4
    prompts = tp_count * seq_local
    cached, asked = tables(length, rope_width)
    tile = 8
    any_space = pl.BlockSpec(memory_space=pl.ANY)
    hbm = pl.BlockSpec(memory_space=pltpu.HBM)
    vmem = pl.BlockSpec(memory_space=pltpu.VMEM)
    count = len(cuts) - 1
    dma = pltpu.SemaphoreType.DMA
    made = pl.pallas_call(
        functools.partial(kernel, sp_count, tp_count, heads_dev, lead, rope_at, cuts, groups, parts),
        out_shape=(
            jax.ShapeDtypeStruct((1, heads_dev, length, key_width), BF16),
            jax.ShapeDtypeStruct((1, heads_dev, length, key_width), BF16),
            jax.ShapeDtypeStruct((1, rope_width, length), BF16),
        ),
        in_specs=[hbm] * 7,
        out_specs=(vmem,) * 3,
        scratch_shapes=[
            pltpu.VMEM((sp_count + prompts, rows, latent_width), BF16),
            pltpu.VMEM(tokens.shape, BF16),
            pltpu.VMEM(kv_down.shape, BF16),
            pltpu.VMEM((rope_width, model_width), BF16),
            pltpu.VMEM((1, latent_width), F32),
            pltpu.VMEM((2, latent_width, tile, key_width), BF16),
            pltpu.VMEM((latent_width * tile, key_width), F32),
            pltpu.VMEM((latent_width, heads_dev * key_width), BF16),
            pltpu.VMEM((latent_width, heads_dev * key_width), BF16),
            pltpu.VMEM((2, rope_width // 2, pos_dev), F32),
            dma((parts + 3,)),
            dma((2,)),
            dma((max(prompts - seq_local, 1), count)),
            dma((len(groups) + 1,)),
            pltpu.SemaphoreType.REGULAR((1,)),
        ],
        compiler_params=pltpu.CompilerParams(
            collective_id=0, has_side_effects=True, vmem_limit_bytes=53000000
        ),
    )(
        *[
            pltpu.with_memory_space_constraint(array, pltpu.HBM)
            for array in (
                tokens, kv_down, rope_down.T, kv_gain.reshape(1, latent_width), key_up, value_up,
                jnp.asarray(cached),
            )
        ]
    )
    key_cache, value_cache, rope_t, read_out = pl.pallas_call(
        functools.partial(finish, (key_width + rope_width) ** (-0.5)),
        out_shape=tuple(jax.ShapeDtypeStruct(part.shape, BF16) for part in made)
        + (jax.ShapeDtypeStruct((1, heads_dev, key_width), BF16),),
        in_specs=[vmem] * 6,
        out_specs=(any_space,) * 4,
        scratch_shapes=[pltpu.VMEM((1, heads_dev, key_width), BF16), dma((4,))],
        compiler_params=pltpu.CompilerParams(vmem_limit_bytes=8 * 1024 * 1024),
    )(*made, query_nope, query_rope, jnp.asarray(asked))
    return (key_cache, value_cache, jnp.swapaxes(rope_t, 1, 2), read_out)


def solution(mesh):
    placed = (
        P(("grp", "tp"), "sp", None),
        P(),
        P(),
        P(),
        P(),
        P(),
        P(("grp", "sp"), "tp", None),
        P(("grp", "sp"), "tp", None),
    )
    return jax.shard_map(
        local,
        mesh=mesh,
        in_specs=placed,
        out_specs=(
            P(("grp", "sp"), "tp", None, None),
            P(("grp", "sp"), "tp", None, None),
            P(("grp", "sp"), None, None),
            P(("grp", "sp"), "tp", None),
        ),
        check_vma=False,
    )
```

```python
import functools

import jax
import jax.numpy as jnp
import numpy as np
from jax import lax
from jax.experimental import pallas as pl
from jax.experimental.pallas import tpu as pltpu
from jax.sharding import PartitionSpec as P

norm_epsilon = 1e-06
rope_base = 10000.0
MESH = pl.DeviceIdType.MESH
F32, BF16 = jnp.float32, jnp.bfloat16


def tables(length, width):
    frequency = (1.0 / rope_base ** (np.arange(0, width, 2, dtype=np.float64) / width)).astype(np.float32)
    angles = frequency[:, None] * np.arange(length, dtype=np.float32)[None, :]
    cached = np.stack([np.cos(angles.astype(np.float64)), np.sin(angles.astype(np.float64))])
    ask = (np.float32(length) * frequency).astype(np.float64)
    asked = np.stack([np.tile(np.cos(ask), 2), np.tile(np.sin(ask), 2)])
    return cached.astype(np.float32), asked.astype(np.float32)


def kernel(
    sp_count, tp_count, heads_dev, lead, rope_at, cuts, groups, parts,
    tok, kvd, rpt, gain, kup, vup, tab,
    key_out, val_out, rope_out,
    box, tok_v, kvd_v, rpt_v, gain_v, up_v, wide, kw, vw, tab_v,
    load_sem, sent, zrecv, crecv, ready,
):
    me = lax.axis_index("sp")
    here = lax.axis_index("tp")
    seq_local, pos_dev, model_width = tok.shape
    latent_width = kvd.shape[1]
    rope_width = rpt.shape[0]
    half = rope_width // 2
    key_width = kup.shape[2]
    rope_rows = box.shape[1] - pos_dev
    rope_packs = rope_width // rope_rows
    pieces = [pl.ds(a, b - a) for a, b in zip(cuts[:-1], cuts[1:])]
    count = len(pieces)
    last = tp_count - 1
    prompts = tp_count * seq_local
    inner = {0: here < last, 1: here > 0}
    ends = {0: here == last, 1: here == 0}
    near_end = {0: here + 1 == last, 1: here - 1 == 0}
    at_end = jnp.logical_or(here == 0, here == last)

    spans = [pl.ds(cuts[g[0]], cuts[g[-1] + 1] - cuts[g[0]]) for g in groups]
    group_of = {s: n for n, g in enumerate(groups) for s in g}

    tile = up_v.shape[2]
    head_start = here * heads_dev
    head_tile = pl.multiple_of(head_start // tile * tile, tile)
    head_off = lax.rem(head_start, tile)
    deep = model_width // parts

    def load(pairs, index):
        size = 0
        for src, dst in pairs:
            pltpu.make_async_copy(src, dst, load_sem.at[index]).start()
            size += int(np.prod(dst.shape)) * dst.dtype.itemsize
        rows = size // (latent_width * kvd_v.dtype.itemsize)
        whole = kvd_v.at[0:rows, :]
        return pltpu.make_async_copy(whole, whole, load_sem.at[index])

    firsts = []
    for n in range(parts):
        span = pl.ds(n * deep, deep)
        firsts.append(load([
            (kvd.at[span, :], kvd_v.at[span, :]),
            (tok.at[:, 0:lead, span], tok_v.at[:, 0:lead, span]),
        ], n))
    gains = pltpu.make_async_copy(gain, gain_v, load_sem.at[parts])
    gains.start()
    following = load([(tok.at[:, lead:rope_at, :], tok_v.at[:, lead:rope_at, :])], parts + 3)
    rest = load([
        (tok.at[:, rope_at:pos_dev, :], tok_v.at[:, rope_at:pos_dev, :]),
        (rpt, rpt_v),
        (tab.at[:, :, pl.ds(pl.multiple_of(me * pos_dev, pos_dev), pos_dev)], tab_v),
    ], parts + 1)
    for n, src in enumerate((kup, vup)):
        pltpu.make_async_copy(
            src.at[:, pl.ds(head_tile, tile), :], up_v.at[n], load_sem.at[parts + 2]
        ).start()

    lanes = [*range(1, sp_count, 2), *range(0, sp_count, 2)]
    barrier = pltpu.get_barrier_semaphore()
    for way in (0, 1):
        @pl.when(inner[way])
        def _(way=way):
            pl.semaphore_signal(
                barrier, inc=1, device_id={"tp": here + (1 if way == 0 else -1)}, device_id_type=MESH
            )
    for step in range(1, sp_count):
        pl.semaphore_signal(
            barrier, inc=1, device_id={"sp": lax.rem(me + step, sp_count)}, device_id_type=MESH
        )

    def landing(lane, group):
        return crecv.at[group + lax.rem(lane, 2) if group == 1 else group + (group > 1)]

    def slot(prompt):
        return jnp.where(prompt == me, me, sp_count + prompt)

    def along(prompt, way, s, final=False):
        part = box.at[slot(prompt), pieces[s]]
        tp = here + (1 if way == 0 else -1)
        if final:
            return pltpu.make_async_remote_copy(
                src_ref=part, dst_ref=box.at[me, pieces[s]],
                send_sem=sent.at[0], recv_sem=landing(me, group_of[s]),
                device_id={"sp": prompt, "tp": tp}, device_id_type=MESH,
            )
        return pltpu.make_async_remote_copy(
            src_ref=part, dst_ref=part,
            send_sem=sent.at[0], recv_sem=zrecv.at[prompt - way * seq_local, s],
            device_id={"sp": me, "tp": tp}, device_id_type=MESH,
        )

    def pass_on(prompt, way, hop, s):
        final = near_end[way] if hop else jnp.logical_and(near_end[way], prompt == me)

        @pl.when(jnp.logical_and(inner[way], final))
        def _():
            along(prompt, way, s, True).start()

        @pl.when(jnp.logical_and(inner[way], jnp.logical_not(final)))
        def _():
            along(prompt, way, s).start()

    def across(prompt, s):
        return pltpu.make_async_remote_copy(
            src_ref=box.at[slot(prompt), pieces[s]], dst_ref=box.at[me, pieces[s]],
            send_sem=sent.at[1], recv_sem=landing(me, group_of[s]),
            device_id={"sp": prompt}, device_id_type=MESH,
        )

    def normed(latent):
        return (
            latent
            * lax.rsqrt(jnp.mean(latent * latent, axis=-1, keepdims=True) + norm_epsilon)
            * gain_v[...]
        ).astype(BF16)

    def send(chosen):
        for s in chosen:
            for q in range(seq_local):
                prompt = here * seq_local + q
                for way in (1, 0):
                    pass_on(prompt, way, 0, s)

                @pl.when(prompt != me)
                def _(s=s):
                    across(prompt, s).start()

    sums = [None] * seq_local
    for n in range(parts):
        firsts[n].wait()
        for q in range(seq_local):
            term = jnp.dot(
                tok_v[q, 0:lead, n * deep:(n + 1) * deep], kvd_v[n * deep:(n + 1) * deep, :],
                preferred_element_type=F32,
            )
            sums[q] = term if n == 0 else sums[q] + term
    gains.wait()
    for q in range(seq_local):
        box[slot(here * seq_local + q), 0:lead, :] = normed(sums[q])
    pl.semaphore_wait(
        barrier, sp_count - 1 + jnp.where(inner[0], 1, 0) + jnp.where(inner[1], 1, 0)
    )
    send((0,))

    for way in (0, 1):
        @pl.when(jnp.logical_and(ends[way], inner[1 - way]))
        def _(way=way):
            pl.semaphore_signal(
                ready.at[0], inc=1, device_id={"tp": here + (-1 if way == 0 else 1)}, device_id_type=MESH
            )

    def finish_rows(begin, stop, place):
        for q in range(seq_local):
            latent = jnp.dot(tok_v[q, begin:stop, :], kvd_v[...], preferred_element_type=F32)
            box[slot(here * seq_local + q), place:place + stop - begin, :] = normed(latent)

    following.wait()
    finish_rows(lead, rope_at, lead)
    send((1,))
    rest.wait()
    finish_rows(rope_at, pos_dev, rope_at + rope_rows)
    for q in range(seq_local):
        raw = lax.dot_general(rpt_v[...], tok_v[q], (((1,), (1,)), ((), ())), preferred_element_type=F32)
        cosine, sine_part = tab_v[0], tab_v[1]
        front, back = raw[:half], raw[half:]
        turned = jnp.concatenate(
            [front * cosine - back * sine_part, front * sine_part + back * cosine], axis=0
        ).astype(BF16)
        box[slot(here * seq_local + q), rope_at:rope_at + rope_rows, :] = jnp.concatenate(
            [turned[g * rope_rows:(g + 1) * rope_rows] for g in range(rope_packs)], axis=1
        )
    send(range(2, count))

    pltpu.make_async_copy(up_v, up_v, load_sem.at[parts + 2]).wait()
    depth = up_v.shape[1]
    for n, target in enumerate((kw, vw)):
        wide[...] = up_v[n].astype(F32).reshape(depth * tile, key_width)
        for h in range(heads_dev):
            target[:, h * key_width:(h + 1) * key_width] = wide[
                pl.ds(head_off + h, depth, stride=tile), :
            ].astype(BF16)

    for way in (0, 1):
        @pl.when(jnp.logical_and(inner[way], near_end[way]))
        def _():
            pl.semaphore_wait(ready.at[0], 1)

    for hop in range(last):
        for s in range(count):
            for q in range(seq_local):
                for way in (1, 0):
                    owner = here - 1 - hop if way == 0 else here + 1 + hop
                    prompt = owner * seq_local + q
                    has = owner >= 0 if way == 0 else owner <= last
                    landed = ends[way] if hop else jnp.logical_and(ends[way], prompt == me)

                    @pl.when(jnp.logical_and(has, jnp.logical_not(landed)))
                    def _(way=way, prompt=prompt):
                        along(prompt, way, s).wait_recv()
                        if hop + 1 < last:
                            pass_on(prompt, way, hop + 1, s)

                        @pl.when(prompt != me)
                        def _():
                            across(prompt, s).start()

    def arrived(members, group):
        def wait(blocks):
            part = box.at[0:blocks, spans[group]]
            pltpu.make_async_remote_copy(
                src_ref=part, dst_ref=part, send_sem=sent.at[1], recv_sem=landing(members[0], group),
                device_id={"sp": me}, device_id_type=MESH,
            ).wait_recv()

        size = len(members)
        own = lax.rem(me, 2) == members[0] % 2 if group == 1 else me >= 0
        every = jnp.logical_or(landed, jnp.logical_not(own))

        @pl.when(every)
        def _():
            wait(size)
        if size > 1:
            @pl.when(jnp.logical_not(every))
            def _():
                wait(size - 1)

    def drain(index, blocks, most):
        for n in range(1, most + 1):
            @pl.when(blocks == n)
            def _(n=n):
                part = box.at[0:n]
                pltpu.make_async_remote_copy(
                    src_ref=part, dst_ref=part, send_sem=sent.at[index], recv_sem=zrecv.at[0, 0],
                    device_id={"sp": me}, device_id_type=MESH,
                ).wait_send()

    def drained():
        upward = jnp.where(inner[0], (here + 1) * seq_local, 0)
        downward = jnp.where(inner[1], (tp_count - here) * seq_local, 0)
        drain(0, upward + downward, (tp_count + 1) * seq_local if tp_count > 1 else 0)
        beside = jnp.logical_or(jnp.logical_not(at_end), jnp.abs(me // seq_local - here) <= 1)
        reach = jnp.where(at_end, min(tp_count, 2) * seq_local, prompts)
        drain(1, reach - jnp.where(beside, 1, 0), prompts)

    landed = jnp.logical_and(at_end, me // seq_local != here)
    for group, members in enumerate(groups):
        begin, stop = cuts[members[0]], cuts[members[-1] + 1]
        with_rope = begin <= rope_at < stop
        ranges = [(begin, rope_at), (rope_at + rope_rows, stop)] if with_rope else [(begin, stop)]
        ranges = [(a, b) for a, b in ranges if b > a]
        height = sum(b - a for a, b in ranges)
        first = begin if begin <= rope_at else begin - rope_rows
        batch = 2
        if group == len(groups) - 1:
            batch = 4
            drained()
        odds = [lane for lane in lanes if lane % 2]
        evens = [lane for lane in lanes if lane % 2 == 0]
        for base in range(0, sp_count, batch):
            sources = lanes[base:base + batch]
            if group != 1 and base == 0:
                arrived(lanes, group)
            if group == 1 and odds[0] in sources:
                arrived(odds, group)
            if group == 1 and evens[0] in sources:
                arrived(evens, group)
            for source in sources:
                if with_rope:
                    packed = box[source, rope_at:rope_at + rope_rows, :]
                    rope_out[0, :, source * pos_dev:(source + 1) * pos_dev] = jnp.concatenate(
                        [packed[:, g * pos_dev:(g + 1) * pos_dev] for g in range(rope_packs)], axis=0
                    )
            rows = jnp.concatenate([box[source, a:b, :] for source in sources for a, b in ranges], axis=0)
            for weight, target in ((kw, key_out), (vw, val_out)):
                made = jnp.dot(rows, weight[...], preferred_element_type=F32).astype(BF16)
                for n, source in enumerate(sources):
                    place = slice(source * pos_dev + first, source * pos_dev + first + height)
                    for h in range(heads_dev):
                        target[0, h, place, :] = made[
                            n * height:(n + 1) * height, h * key_width:(h + 1) * key_width
                        ]


def finish(scale, keys, vals, ropes, query, ask, qtab, key_out, val_out, rope_out, read_out, read, sem):
    heads_dev, key_width = query.shape[1], query.shape[2]
    moves = [
        pltpu.make_async_copy(src, dst, sem.at[n])
        for n, (src, dst) in enumerate([(keys, key_out), (vals, val_out), (ropes, rope_out)])
    ]
    for move in moves:
        move.start()
    half = ask.shape[2] // 2
    turn = ask[0].astype(F32)
    swapped = jnp.concatenate([-turn[:, half:], turn[:, :half]], axis=1)
    rotated = (turn * qtab[0:1, :] + swapped * qtab[1:2, :]).astype(BF16)
    shape = (heads_dev, heads_dev * key_width)
    own = lax.broadcasted_iota(jnp.int32, shape, 1) // key_width == lax.broadcasted_iota(jnp.int32, shape, 0)
    spread = jnp.where(own, jnp.concatenate([query[0].astype(F32)] * heads_dev, axis=1), 0.0).astype(BF16)
    all_keys = jnp.concatenate([keys[0, h] for h in range(heads_dev)], axis=1)
    total = lax.dot_general(spread, all_keys, (((1,), (1,)), ((), ())), preferred_element_type=F32)
    total = (total + jnp.dot(rotated, ropes[0], preferred_element_type=F32)) * scale
    terms = jnp.exp(total - jnp.max(total, axis=-1, keepdims=True))
    high = terms.astype(BF16).astype(F32)
    both = jnp.concatenate([high, terms - high], axis=0).astype(BF16)
    all_vals = jnp.concatenate([vals[0, h] for h in range(heads_dev)], axis=1)
    reads = jnp.dot(both, all_vals, preferred_element_type=F32)
    picks = []
    for h in range(heads_dev):
        span = slice(h * key_width, (h + 1) * key_width)
        picks.append(reads[h:h + 1, span] + reads[heads_dev + h:heads_dev + h + 1, span])
    read[0] = (jnp.concatenate(picks, axis=0) / jnp.sum(terms, axis=-1, keepdims=True)).astype(BF16)
    moves.append(pltpu.make_async_copy(read, read_out, sem.at[3]))
    moves[-1].start()
    for move in moves:
        move.wait()


def local(tokens, kv_down, rope_down, kv_gain, key_up, value_up, query_nope, query_rope):
    seq_local, pos_dev, model_width = tokens.shape
    sp_count = lax.axis_size("sp")
    tp_count = lax.axis_size("tp")
    latent_width = kv_down.shape[1]
    rope_width = rope_down.shape[1]
    head_count, key_width = key_up.shape[1], key_up.shape[2]
    heads_dev = head_count // tp_count
    length = pos_dev * sp_count
    rope_rows = rope_width * pos_dev // latent_width
    rows = rope_rows + pos_dev
    quarter = pos_dev // 4
    lead, rope_at = quarter, 2 * quarter
    cuts = (0, lead, rope_at, rows - quarter // 2, rows)
    groups = ((0, 1), (2,), (3,))
    parts = 4
    prompts = tp_count * seq_local
    cached, asked = tables(length, rope_width)
    tile = 8
    any_space = pl.BlockSpec(memory_space=pl.ANY)
    hbm = pl.BlockSpec(memory_space=pltpu.HBM)
    vmem = pl.BlockSpec(memory_space=pltpu.VMEM)
    count = len(cuts) - 1
    dma = pltpu.SemaphoreType.DMA
    made = pl.pallas_call(
        functools.partial(kernel, sp_count, tp_count, heads_dev, lead, rope_at, cuts, groups, parts),
        out_shape=(
            jax.ShapeDtypeStruct((1, heads_dev, length, key_width), BF16),
            jax.ShapeDtypeStruct((1, heads_dev, length, key_width), BF16),
            jax.ShapeDtypeStruct((1, rope_width, length), BF16),
        ),
        in_specs=[hbm] * 7,
        out_specs=(vmem,) * 3,
        scratch_shapes=[
            pltpu.VMEM((sp_count + prompts, rows, latent_width), BF16),
            pltpu.VMEM(tokens.shape, BF16),
            pltpu.VMEM(kv_down.shape, BF16),
            pltpu.VMEM((rope_width, model_width), BF16),
            pltpu.VMEM((1, latent_width), F32),
            pltpu.VMEM((2, latent_width, tile, key_width), BF16),
            pltpu.VMEM((latent_width * tile, key_width), F32),
            pltpu.VMEM((latent_width, heads_dev * key_width), BF16),
            pltpu.VMEM((latent_width, heads_dev * key_width), BF16),
            pltpu.VMEM((2, rope_width // 2, pos_dev), F32),
            dma((parts + 4,)),
            dma((2,)),
            dma((max(prompts - seq_local, 1), count)),
            dma((len(groups) + 1,)),
            pltpu.SemaphoreType.REGULAR((1,)),
        ],
        compiler_params=pltpu.CompilerParams(
            collective_id=0, has_side_effects=True, vmem_limit_bytes=53000000
        ),
    )(
        *[
            pltpu.with_memory_space_constraint(array, pltpu.HBM)
            for array in (
                tokens, kv_down, rope_down.T, kv_gain.reshape(1, latent_width), key_up, value_up,
                jnp.asarray(cached),
            )
        ]
    )
    key_cache, value_cache, rope_t, read_out = pl.pallas_call(
        functools.partial(finish, (key_width + rope_width) ** (-0.5)),
        out_shape=tuple(jax.ShapeDtypeStruct(part.shape, BF16) for part in made)
        + (jax.ShapeDtypeStruct((1, heads_dev, key_width), BF16),),
        in_specs=[vmem] * 6,
        out_specs=(any_space,) * 4,
        scratch_shapes=[pltpu.VMEM((1, heads_dev, key_width), BF16), dma((4,))],
        compiler_params=pltpu.CompilerParams(vmem_limit_bytes=8 * 1024 * 1024),
    )(*made, query_nope, query_rope, jnp.asarray(asked))
    return (key_cache, value_cache, jnp.swapaxes(rope_t, 1, 2), read_out)


def solution(mesh):
    placed = (
        P(("grp", "tp"), "sp", None),
        P(),
        P(),
        P(),
        P(),
        P(),
        P(("grp", "sp"), "tp", None),
        P(("grp", "sp"), "tp", None),
    )
    return jax.shard_map(
        local,
        mesh=mesh,
        in_specs=placed,
        out_specs=(
            P(("grp", "sp"), "tp", None, None),
            P(("grp", "sp"), "tp", None, None),
            P(("grp", "sp"), None, None),
            P(("grp", "sp"), "tp", None),
        ),
        check_vma=False,
    )
```
